128 devices in a mesh: sp: 64 (over z, y, x), tp: 2 (over core).
Axes of the slice: x: 4, y: 4, z: 4, core: 2. Of those that a mesh axis runs over, the one named last changes fastest.
Arguments:
- cotangent: bfloat16 [12288, 2048], P('sp'), may hold values from -1.75 to 1.75
- mixed_input: bfloat16 [12288, 2048], P('sp'), may hold values from -6 to 6
- route_ids: int32 [12288, 2], P('sp'), may hold values from 0 to 63, all different within a row; in each aligned block of 192 rows (0 to 191, 192 to 383, ...) at most 12 rows name the same one
- route_gates: float32 [12288, 2], P('sp'), may hold values from 0.25 to 1.5
- expert_gate: bfloat16 [64, 2048, 1024], P('sp', None, 'tp'), may hold values from -0.125 to 0.125
- expert_up: bfloat16 [64, 2048, 1024], P('sp', None, 'tp'), may hold values from -0.125 to 0.125
- expert_down: bfloat16 [64, 1024, 2048], P('sp', 'tp'), may hold values from -0.1875 to 0.1875
- projection: bfloat16 [2048, 1024], P(None, 'tp'), may hold values from -0.1875 to 0.1875
- mixer_output: bfloat16 [12288, 1024], P('sp', 'tp'), may hold values from -6 to 6
- query_rows: bfloat16 [12288, 512], P('sp', 'tp'), may hold values from -6 to 6
- key_rows: bfloat16 [12288, 512], P('sp', 'tp'), may hold values from -0.75 to 0.75
- value_rows: bfloat16 [12288, 1024], P('sp', 'tp'), may hold values from -6 to 6
- log_forward: float32 [12288, 512], P('sp', 'tp'), may hold values from -0.25 to 0, as said below
- log_backward: float32 [12288, 512], P('sp', 'tp'), may hold values from -0.25 to 0, as said below
Outputs:
- gate_grad: float32 [64, 2048, 1024], P('sp', None, 'tp')
- up_grad: float32 [64, 2048, 1024], P('sp', None, 'tp')
- down_grad: float32 [64, 1024, 2048], P('sp', 'tp')
- projection_grad: float32 [2048, 1024], P('sp', 'tp')
- query_grad: float32 [12288, 512], P('sp', 'tp')
- key_grad: float32 [12288, 512], P('sp', 'tp')
- value_grad: float32 [12288, 1024], P('sp', 'tp')
- log_forward_grad: float32 [12288, 512], P('sp', 'tp')
- log_backward_grad: float32 [12288, 512], P('sp', 'tp')
The draws below stay inside these ranges and needn't reach their ends.
Inputs may be any that keep to these rules, and one draw needn't show every extreme that they name: `route_ids`: in the rows of one device no expert is named by more than 12 routes, a bound that some block reaches in the rows of some device; the 2 experts of a token differ. `log_forward`: strictly negative. `log_backward`: strictly negative.
All inputs are finite; a program needn't handle non-finite values.
Results may differ from the reference program's by a relative error of at most 0.006.
Values may be sent and summed in bfloat16 or wider, within the bound.
A program may use at most 192 MiB of HBM per device.

```python
import math
import jax
import jax.numpy as jnp
import numpy as np
from jax import lax

D = 2048
F = 1024
HEADS = 16
DK = 32
DV = 64
BLK = 64
TOP = 2
TOK_DEV = 192
TOKENS = 12288
EXPERTS = 64
CAP = 12
QW = 512
VW = 1024
N_SP = 64
N_TP = 2


def decay_table(base_key):
    subkeys = jax.random.split(base_key, 6)
    slow_share = 0.5
    slow_mask = jax.random.uniform(subkeys[0], (QW,), jnp.float32) < slow_share
    slow_rate = jnp.exp(jax.random.uniform(subkeys[1], (QW,), jnp.float32, math.log(0.3), math.log(1.5))) / TOKENS
    fast_rate = jnp.exp(jax.random.uniform(subkeys[2], (QW,), jnp.float32, math.log(0.01), math.log(1.0 / 30.0)))
    rates = jnp.where(slow_mask, slow_rate, fast_rate)
    block_factor = jnp.repeat(jnp.exp(jax.random.uniform(subkeys[3], (TOKENS // BLK, QW), jnp.float32, -0.7, 0.7)), BLK, axis=0)
    device_factor = jnp.repeat(jnp.exp(jax.random.uniform(subkeys[4], (TOKENS // TOK_DEV, QW), jnp.float32, -0.7, 0.7)), TOK_DEV, axis=0)
    roughness = jax.random.uniform(subkeys[5], (TOKENS, QW), jnp.float32, 0.5, 1.5)
    return -(rates[None, :] * block_factor * device_factor * roughness)


def draw_log_forward(key, part):
    return decay_table(jax.random.fold_in(key, 11))


def draw_log_backward(key, part):
    return decay_table(jax.random.fold_in(key, 12))


def raised(entries, key, source, target, shards_of, factor):
    owner, partner = [(jnp.arange(entries.shape[axis_at]) // (entries.shape[axis_at] // shards_of)).reshape([-1 if axis == axis_at else 1 for axis in range(entries.ndim)]) for axis_at in (source, target)]
    chosen = jax.random.permutation(key, shards_of)[partner]
    strong = (owner == chosen) | (owner == (partner + shards_of // 2) % shards_of)
    return jnp.where(strong, factor * entries, entries)


def block_levels(own_key, dims, pieces, low, largest):
    loudness = 1.0
    for dim, blocks in pieces:
        draws = jax.random.uniform(jax.random.fold_in(jax.random.fold_in(own_key, 6), dim), (blocks,), jnp.float32, low / len(pieces), largest / len(pieces))
        loudness = loudness * jnp.repeat(jnp.exp(draws), dims[dim] // blocks).reshape((-1,) + (1,) * (len(dims) - 1 - dim))
    return loudness


def deal_out(own_key, own, number, rows, count, top, reach, lean):
    ranking = jax.random.permutation(own_key, count)
    heavy_load, usual = load_shares(count, rows * top, reach, lean, True), load_shares(count, rows * top, reach, lean, False)
    places = jnp.arange(count)

    def named(lengths, offset_by):
        used = int((lengths > 0).sum())
        fixed = max(1, used // 4)
        shifted = fixed + (places - fixed + offset_by * (used - fixed)) % max(1, count - fixed)
        return jnp.zeros((count,), jnp.int32).at[ranking[jnp.where(places < fixed, places, shifted)]].set(jnp.asarray(lengths, jnp.int32))

    lengths = jnp.where(number % 4 == 0, named(heavy_load, number // 4), named(usual, number - number // 4 - 1))
    mixed = jax.random.permutation(jax.random.fold_in(own, 3), count)
    giver, receiver = mixed[0:count // 2 * 2:2], mixed[1:count // 2 * 2:2]
    margin = jnp.minimum(lengths[giver] - 1, reach - lengths[receiver]) // 2
    margin = jnp.where((giver == ranking[0]) | (receiver == ranking[0]) | (lengths[receiver] == 0), 0, jnp.maximum(margin, 0))
    shifted = jax.random.randint(jax.random.fold_in(own, 4), (count // 2,), 0, 1 << 20) % (margin + 1)
    lengths = lengths.at[giver].add(-shifted).at[receiver].add(shifted)
    labels = jnp.searchsorted(jnp.cumsum(lengths), jnp.arange(rows * top), side="right").astype(jnp.int32)
    table = labels.reshape(top, rows).T
    table = table[jax.random.permutation(jax.random.fold_in(own, 1), rows)]
    offset_by = jax.random.randint(jax.random.fold_in(own, 2), (rows, 1), 0, top)
    return jnp.take_along_axis(table, (jnp.arange(top)[None, :] + offset_by) % top, axis=1)


def load_shares(amount, total, bound, skew, full):
    loads = [(1 << 20) // math.isqrt(standing ** skew) + 1 for standing in range(1, amount + 1)]
    largest = bound if full else min(bound, max(-(-total // amount), total * loads[0] // sum(loads)))
    least = 1 if total - largest >= amount - 1 else 0
    counts, spare = [largest] + [least] * (amount - 1), total - largest - least * (amount - 1)
    while spare > 0:
        candidates = [i for i in range(1, amount) if counts[i] < largest] or [i for i in range(1, amount) if counts[i] < bound]
        mass, remaining = sum([loads[i] for i in candidates]), spare
        for i in candidates:
            addition = min(bound - counts[i], max(1, remaining * loads[i] // mass), spare)
            counts[i] = counts[i] + addition
            spare = spare - addition
    return np.array(counts)


def normal_values(key, shape, scale, limit, cuts=(), held_as=jnp.bfloat16):
    values = scale * jax.random.normal(key, shape, jnp.float32)
    if cuts:
        values = values * block_levels(key, shape, cuts, -0.22, 0.18)
    return jnp.clip(values, -limit, limit).astype(held_as)


def heavy_noise(own_key, shape, width, most, shards, heavy, kind=jnp.bfloat16):
    values = width * jax.random.normal(own_key, shape, jnp.float32)
    if shards:
        values = values * block_levels(own_key, shape, shards, -0.22, 0.18)
    return jnp.clip(raised(values, jax.random.fold_in(own_key, 3), *heavy), -most, most).astype(kind)


def setup_inputs(seed: int = 0) -> dict:
    arg_keys = jax.random.split(jax.random.key(seed), 15)
    cotangent = heavy_noise(arg_keys[0], (TOKENS, D), 0.1, 1.75, ((0, 64),), (0, 1, 64, 4.0))
    mixed_input = normal_values(arg_keys[1], (TOKENS, D), 1.0, 6.0, ((0, 64),))
    route_ids_keys = jax.random.split(jax.random.fold_in(arg_keys[2], 1), TOKENS // TOK_DEV)
    route_ids_turns = jax.random.permutation(jax.random.fold_in(arg_keys[2], 3), TOKENS // TOK_DEV)
    route_ids = jax.vmap(lambda own, number: deal_out(jax.random.fold_in(arg_keys[2], 2), own, number, TOK_DEV, EXPERTS, TOP, CAP, 2))(route_ids_keys, route_ids_turns).reshape((TOKENS, TOP))
    route_gates = jnp.clip(0.25 + 1.25 * jax.random.uniform(arg_keys[3], (TOKENS, TOP), jnp.float32) ** block_levels(arg_keys[3], (TOKENS, TOP), ((0, 64),), -0.2, 0.2), 0.25, 1.5)
    expert_gate = normal_values(arg_keys[4], (EXPERTS, D, F), D ** -0.5, 0.125, ((0, 64), (2, 2)))
    expert_up = normal_values(arg_keys[5], (EXPERTS, D, F), D ** -0.5, 0.125, ((0, 64), (2, 2)))
    expert_down = normal_values(arg_keys[6], (EXPERTS, F, D), F ** -0.5, 0.1875, ((0, 64), (1, 2)))
    projection = normal_values(arg_keys[7], (D, VW), VW ** -0.5, 0.1875, ((1, 2),))
    mixer_output = normal_values(arg_keys[8], (TOKENS, VW), 1.0, 6.0, ((0, 64), (1, 2)))
    query_rows = normal_values(arg_keys[9], (TOKENS, QW), 1.0, 6.0, ((0, 64), (1, 2)))
    key_rows = normal_values(arg_keys[10], (TOKENS, QW), 0.125, 0.75, ((0, 64), (1, 2)))
    value_rows = normal_values(arg_keys[11], (TOKENS, VW), 1.0, 6.0, ((0, 64), (1, 2)))
    log_forward = draw_log_forward(jax.random.fold_in(arg_keys[14], 71), 0)
    log_backward = draw_log_backward(jax.random.fold_in(arg_keys[14], 71), 0)
    return {"cotangent": cotangent, "mixed_input": mixed_input, "route_ids": route_ids, "route_gates": route_gates, "expert_gate": expert_gate, "expert_up": expert_up, "expert_down": expert_down, "projection": projection, "mixer_output": mixer_output, "query_rows": query_rows, "key_rows": key_rows, "value_rows": value_rows, "log_forward": log_forward, "log_backward": log_backward}


topmost_precision = lax.Precision.HIGHEST

def decayed_pass(query_stack, key_matrix, value_matrix, log_rate, entering):
    count = query_stack.shape[0]
    head_count = query_stack.shape[1]
    key_width = query_stack.shape[2]
    value_width = value_matrix.shape[2]
    blocks = count // BLK
    query_blocks = query_stack.reshape(blocks, BLK, head_count, key_width)
    key_blocks = key_matrix.reshape(blocks, BLK, head_count, key_width)
    value_blocks = value_matrix.reshape(blocks, BLK, head_count, value_width)
    running_prefix = jnp.cumsum(log_rate.reshape(blocks, BLK, head_count, key_width), axis=1)
    last_cum = running_prefix[:, -1:]
    increment = jnp.einsum('nlhk,nlhv->nhkv', key_blocks * jnp.exp(last_cum - running_prefix), value_blocks, precision=topmost_precision)
    decay = jnp.exp(last_cum[:, 0])

    def advance(carried, inputs):
        factor, added = inputs
        return (factor[..., None] * carried + added, carried)
    final_state, entering_states = lax.scan(advance, entering, (decay, increment))
    inter_part = jnp.einsum('nlhk,nhkv->nlhv', query_blocks * jnp.exp(running_prefix), entering_states, precision=topmost_precision)
    middle = running_prefix[:, BLK // 2 - 1:BLK // 2]
    scores = jnp.einsum('nlhk,nmhk->nhlm', query_blocks * jnp.exp(running_prefix - middle), key_blocks * jnp.exp(middle - running_prefix), precision=topmost_precision)
    lower_mask = jnp.tril(jnp.ones((BLK, BLK), bool))
    scores = jnp.where(lower_mask, scores, jnp.float32(0.0))
    intra_part = jnp.einsum('nhlm,nmhv->nlhv', scores, value_blocks, precision=topmost_precision)
    return ((inter_part + intra_part).reshape(count, head_count, value_width), final_state)

def reverse_rows(source_array):
    return jnp.flip(source_array, axis=0)

def whole_mixer(query_in, key_in, value_in, forward_in, backward_in):
    query_scaling = DK ** (-0.5)
    entering = jnp.zeros((HEADS, DK, DV), jnp.float32)
    out_fwd, _ = decayed_pass(query_in * query_scaling, key_in, value_in, forward_in, entering)
    out_bwd, _ = decayed_pass(reverse_rows(query_in) * query_scaling, reverse_rows(key_in), reverse_rows(value_in), reverse_rows(backward_in), entering)
    return out_fwd + reverse_rows(out_bwd)

def reference(cotangent, mixed_input, route_ids, route_gates, expert_gate, expert_up, expert_down, projection, mixer_output, query_rows, key_rows, value_rows, log_forward, log_backward):
    flat_ids = route_ids.reshape(-1)
    route_total = TOKENS * TOP
    row_limit = N_SP * CAP
    unit_share = F // N_TP
    gate_padded = jnp.concatenate([route_gates.reshape(-1), jnp.zeros((1,), jnp.float32)])
    cot_padded = jnp.concatenate([cotangent, jnp.zeros((1, D), jnp.bfloat16)], axis=0)
    input_padded = jnp.concatenate([mixed_input, jnp.zeros((1, D), jnp.bfloat16)], axis=0)

    def per_expert(gathered_sum, expert_index):
        found = jnp.nonzero(flat_ids == expert_index, size=row_limit, fill_value=route_total)[0].astype(jnp.int32)
        token_of = (found // TOP).astype(jnp.int32)
        routed = (gate_padded[found][:, None] * cot_padded[token_of].astype(jnp.float32)).astype(jnp.bfloat16)
        tok_rows = input_padded[token_of]
        w_gate = expert_gate[expert_index]
        w_up = expert_up[expert_index]
        w_down = expert_down[expert_index]
        gate_pre = jnp.dot(tok_rows, w_gate, preferred_element_type=jnp.float32)
        up_pre = jnp.dot(tok_rows, w_up, preferred_element_type=jnp.float32)
        sigmoid_gate = jax.nn.sigmoid(gate_pre)
        silu_gate = gate_pre * sigmoid_gate
        hidden = (silu_gate * up_pre).astype(jnp.bfloat16)
        hidden_grad = jnp.dot(routed, w_down.T, preferred_element_type=jnp.float32)
        slope = sigmoid_gate * (1.0 + gate_pre * (1.0 - sigmoid_gate))
        gate_pre_grad = (hidden_grad * up_pre * slope).astype(jnp.bfloat16)
        up_pre_grad = (hidden_grad * silu_gate).astype(jnp.bfloat16)
        down_term = jnp.dot(hidden.T, routed, preferred_element_type=jnp.float32)
        gate_term = jnp.dot(tok_rows.T, gate_pre_grad, preferred_element_type=jnp.float32)
        up_term = jnp.dot(tok_rows.T, up_pre_grad, preferred_element_type=jnp.float32)
        row_grad = jnp.zeros((row_limit, D), jnp.float32)
        for portion in range(N_TP):
            start_unit = portion * unit_share
            end_unit = start_unit + unit_share
            partial_value = jnp.dot(gate_pre_grad[:, start_unit:end_unit], w_gate[:, start_unit:end_unit].T, preferred_element_type=jnp.float32)
            partial_value = partial_value + jnp.dot(up_pre_grad[:, start_unit:end_unit], w_up[:, start_unit:end_unit].T, preferred_element_type=jnp.float32)
            rounded = lax.optimization_barrier(partial_value.astype(jnp.bfloat16))
            row_grad = row_grad + rounded.astype(jnp.float32)
        row_grad = row_grad.astype(jnp.bfloat16)
        gathered_sum = gathered_sum.at[token_of].add(row_grad.astype(jnp.float32))
        return (gathered_sum, (gate_term, up_term, down_term))
    gathered, expert_terms = lax.scan(per_expert, jnp.zeros((TOKENS + 1, D), jnp.float32), jnp.arange(EXPERTS, dtype=jnp.int32))
    mid_grad = (gathered[:TOKENS] + cotangent.astype(jnp.float32)).astype(jnp.bfloat16)
    mix_grad = jnp.dot(mid_grad, projection, preferred_element_type=jnp.float32).astype(jnp.bfloat16)
    projection_grad = jnp.dot(mid_grad.T, mixer_output, preferred_element_type=jnp.float32)

    def by_heads(source_array, head_width):
        return source_array.astype(jnp.float32).reshape(TOKENS, HEADS, head_width)
    _, pullback = jax.vjp(whole_mixer, by_heads(query_rows, DK), by_heads(key_rows, DK), by_heads(value_rows, DV), by_heads(log_forward, DK), by_heads(log_backward, DK))
    grads = pullback(by_heads(mix_grad, DV))
    query_grad = grads[0].reshape(TOKENS, QW)
    key_grad = grads[1].reshape(TOKENS, QW)
    value_grad = grads[2].reshape(TOKENS, VW)
    log_forward_grad = grads[3].reshape(TOKENS, QW)
    log_backward_grad = grads[4].reshape(TOKENS, QW)
    return (expert_terms[0], expert_terms[1], expert_terms[2], projection_grad, query_grad, key_grad, value_grad, log_forward_grad, log_backward_grad)
```

```python
import functools

import jax
import jax.numpy as jnp
import numpy as np
from jax import lax
from jax.experimental import pallas as pl
from jax.experimental.pallas import tpu as pltpu
from jax.sharding import PartitionSpec as P

MESH = pl.DeviceIdType.MESH
BF = jnp.bfloat16
F32 = jnp.float32
NSP = 64
CAP = 12
TOK = 192
D = 2048
HD = 1024
FL = 512
NT = (((1,), (1,)), ((), ()))
TN = (((0,), (0,)), ((), ()))
NN = (((1,), (0,)), ((), ()))
ANY = pl.BlockSpec(memory_space=pl.ANY)
VM = pl.BlockSpec(memory_space=pltpu.VMEM)


def mm(a, b, dims=NN):
    return lax.dot_general(a, b, dims, preferred_element_type=F32)


def comps(k):
    return (k // 16, (k // 4) % 4, k % 4)


def shifted(me, off):
    z, y, x = me // 16, (me // 4) % 4, me % 4
    dz, dy, dx = off
    return ((z + dz) % 4) * 16 + ((y + dy) % 4) * 4 + (x + dx) % 4


def neg(k):
    a, b, c = comps(k)
    return ((-a) % 4) * 16 + ((-b) % 4) * 4 + (-c) % 4


def turned(k):
    a, b, c = comps(k)
    return b * 16 + c * 4 + a


def send_order():
    far = sorted(range(1, NSP), key=lambda k: -sum(min(a, 4 - a) for a in comps(k)))
    out = []
    for k in far:
        k2, k3 = turned(k), turned(turned(k))
        for q in (k, neg(k), k2, neg(k2), k3, neg(k3)):
            if q not in out:
                out.append(q)
    return out


ORDER = send_order()


def announce(sp, tp, barrier):
    def signal(k, c):
        pl.semaphore_signal(
            barrier, inc=1, device_id={"sp": shifted(sp, comps(k))}, device_id_type=MESH
        )
        return c

    lax.fori_loop(1, NSP, signal, 0)
    pl.semaphore_signal(barrier, inc=1, device_id={"tp": 1 - tp}, device_id_type=MESH)


def slot_codes(ids, bound):
    expert = lax.broadcasted_iota(jnp.int32, (NSP, TOK), 0).astype(F32)
    before = (
        lax.broadcasted_iota(jnp.int32, (TOK, TOK), 0)
        < lax.broadcasted_iota(jnp.int32, (TOK, TOK), 1)
    ).astype(F32).astype(BF)
    o0 = (expert == ids[0:1]).astype(F32)
    o1 = (expert == ids[1:2]).astype(F32)
    r0 = jnp.sum(o0 * mm(o0.astype(BF), before), axis=0, keepdims=True)
    c0 = jnp.sum(o0, axis=1, keepdims=True)
    r1 = jnp.sum(o1 * (mm(o1.astype(BF), before) + c0), axis=0, keepdims=True)
    return ids[0:1] * bound + r0, ids[1:2] * bound + r1


def expert_kernel(
    ids_ref, gates_ref, code_ref, back_ref, cot_hbm, mix_hbm, wg_hbm, wu_hbm, wd_hbm,
    c_out, t_out, h_out, g_out, u_out, mid_out,
    cot, mix, wg, wu, wd, xs, ra, rb, co, ct, to, tt, hid, gpg, upg, pown, poth, pin, ret, rr, mid, midp,
    ld, ssem, rsem, fs, fr, ps, pr, bs, br, ms, mr, od,
):
    sp, tp = lax.axis_index("sp"), lax.axis_index("tp")
    mine = pl.ds(pl.multiple_of(tp * HD, HD), HD)
    other = pl.ds(pl.multiple_of((1 - tp) * HD, HD), HD)
    loads = [
        pltpu.make_async_copy(cot_hbm.at[:, mine], cot, ld.at[0]),
        pltpu.make_async_copy(mix_hbm.at[:, mine], mix, ld.at[1]),
        pltpu.make_async_copy(wg_hbm, wg, ld.at[2]),
        pltpu.make_async_copy(wu_hbm, wu, ld.at[3]),
        pltpu.make_async_copy(wd_hbm, wd, ld.at[4]),
    ]
    for c in loads:
        c.start()
    barrier = pltpu.get_barrier_semaphore()
    announce(sp, tp, barrier)
    ids = ids_ref[...].astype(F32)
    d0, d1 = slot_codes(ids, float(CAP))
    g0, g1 = gates_ref[0:1], gates_ref[1:2]
    loads[0].wait()
    loads[1].wait()

    def pack(i, c):
        code = code_ref[pl.ds(i * 192, 192), :]
        cc, tc = code[:, 0:1], code[:, 1:2]
        m0, m1 = cc == d0, cc == d1
        selc = (m0 | m1).astype(F32).astype(BF)
        selt = ((tc == d0) | (tc == d1)).astype(F32).astype(BF)
        gate = jnp.sum(jnp.where(m0, g0, 0.0) + jnp.where(m1, g1, 0.0), axis=1, keepdims=True)
        gate = gate + (tc >= 0.0).astype(F32)
        rows = (mm(selc, cot[...]) + mm(selt, mix[...])) * gate
        xs[pl.ds(i * 24, 24)] = rows.reshape(24, 8, HD).astype(BF)
        return c

    lax.fori_loop(0, 8, pack, 0)
    pl.semaphore_wait(barrier, NSP)

    def out_copy(k):
        d = shifted(sp, comps(k))
        return pltpu.make_async_remote_copy(
            src_ref=xs.at[pl.ds(3 * d, 3)], dst_ref=ra.at[pl.ds(3 * sp, 3)],
            send_sem=ssem.at[k], recv_sem=rsem.at[k],
            device_id={"sp": d}, device_id_type=MESH,
        )

    def pass_copy(k):
        s = shifted(sp, comps(neg(k)))
        return pltpu.make_async_remote_copy(
            src_ref=ra.at[pl.ds(3 * s, 3)], dst_ref=rb.at[pl.ds(3 * s, 3)],
            send_sem=fs.at[k], recv_sem=fr.at[k],
            device_id={"tp": 1 - tp}, device_id_type=MESH,
        )

    for k in ORDER:
        out_copy(k).start()
    ra[pl.ds(3 * sp, 3)] = xs[pl.ds(3 * sp, 3)]
    pass_copy(0).start()
    for k in ORDER:
        out_copy(k).wait_recv()
        pass_copy(k).start()
    loads[2].wait()
    loads[3].wait()
    loads[4].wait()
    for k in [0] + ORDER:
        pass_copy(k).wait_recv()

    def split(buf, i, cdst, tdst):
        x = buf[pl.ds(i * 48, 48)].astype(F32).reshape(8, 6, 8, HD)
        a, b = x[:, 2], x[:, 5]
        cm = jnp.concatenate([a[:, 0:4], b[:, 0:4]], axis=1)
        tm = jnp.concatenate([a[:, 4:8], b[:, 4:8]], axis=1)
        cv = jnp.stack([x[:, 0], x[:, 3], cm], axis=1).reshape(192, HD)
        tv = jnp.stack([x[:, 1], x[:, 4], tm], axis=1).reshape(192, HD)
        cdst[pl.ds(i * 192, 192), :] = cv.astype(BF)
        tdst[pl.ds(i * 192, 192), :] = tv.astype(BF)

    def parts(i, c):
        split(ra, i, co, to)
        split(rb, i, ct, tt)
        return c

    lax.fori_loop(0, 4, parts, 0)
    outs = [
        pltpu.make_async_copy(co, c_out.at[:, mine], od.at[0]),
        pltpu.make_async_copy(ct, c_out.at[:, other], od.at[1]),
        pltpu.make_async_copy(to, t_out.at[:, mine], od.at[2]),
        pltpu.make_async_copy(tt, t_out.at[:, other], od.at[3]),
    ]
    for c in outs:
        c.start()

    def chunk(i, c):
        rows = pl.ds(i * 384, 384)
        t1, t2, c1, c2 = to[rows, :], tt[rows, :], co[rows, :], ct[rows, :]
        gate_pre = mm(t1, wg[mine, :]) + mm(t2, wg[other, :])
        up_pre = mm(t1, wu[mine, :]) + mm(t2, wu[other, :])
        hidden_grad = mm(c1, wd[:, mine], NT) + mm(c2, wd[:, other], NT)
        sg = jax.nn.sigmoid(gate_pre)
        silu = gate_pre * sg
        hid[rows, :] = (silu * up_pre).astype(BF)
        slope = sg * (1.0 + gate_pre * (1.0 - sg))
        gg = (hidden_grad * up_pre * slope).astype(BF)
        ug = (hidden_grad * silu).astype(BF)
        gpg[rows, :] = gg
        upg[rows, :] = ug
        poth[rows, :] = (mm(gg, wg[other, :], NT) + mm(ug, wu[other, :], NT)).astype(BF)
        pown[rows, :] = (mm(gg, wg[mine, :], NT) + mm(ug, wu[mine, :], NT)).astype(BF)
        return c

    lax.fori_loop(0, 2, chunk, 0)
    outs2 = [
        pltpu.make_async_copy(hid, h_out, od.at[4]),
        pltpu.make_async_copy(gpg, g_out, od.at[5]),
        pltpu.make_async_copy(upg, u_out, od.at[6]),
    ]
    for c in outs2:
        c.start()
    swap = pltpu.make_async_remote_copy(
        src_ref=poth, dst_ref=pin, send_sem=ps, recv_sem=pr,
        device_id={"tp": 1 - tp}, device_id_type=MESH,
    )
    swap.start()
    swap.wait_recv()

    def sums(i, c):
        rows = pl.ds(i * 192, 192)
        v = (pown[rows, :].astype(F32) + pin[rows, :].astype(F32)).reshape(8, 3, 8, HD)
        m = v[:, 2]
        e = jnp.concatenate([m[:, 0:4, 0:512], m[:, 0:4, 512:1024]], axis=1)
        o = jnp.concatenate([m[:, 4:8, 0:512], m[:, 4:8, 512:1024]], axis=1)
        ev = jnp.concatenate([v[:, 0], e], axis=2)
        ov = jnp.concatenate([v[:, 1], o], axis=2)
        ret[pl.ds(i * 16, 16)] = jnp.stack([ev, ov], axis=1).reshape(16, 8, 1536).astype(BF)
        return c

    lax.fori_loop(0, 4, sums, 0)

    def back_copy(k):
        d = shifted(sp, comps(k))
        return pltpu.make_async_remote_copy(
            src_ref=ret.at[d], dst_ref=rr.at[sp],
            send_sem=bs.at[k], recv_sem=br.at[k],
            device_id={"sp": d}, device_id_type=MESH,
        )

    for k in ORDER:
        back_copy(k).start()
    rr[sp] = ret[sp]
    bc = back_ref[...]
    e0 = ((bc[:, 0:1] == d0) | (bc[:, 0:1] == d1)).astype(F32).astype(BF)
    e1 = ((bc[:, 1:2] == d0) | (bc[:, 1:2] == d1)).astype(F32).astype(BF)
    e2 = ((bc[:, 2:3] == d0) | (bc[:, 2:3] == d1)).astype(F32).astype(BF)
    for k in ORDER:
        back_copy(k).wait_recv()
    full = rr[...].reshape(512, 1536)
    late = full[:, 1024:1536]
    acc = mm(e0, full[:, 0:1024], TN)
    lo, hi = mm(e1, late, TN), mm(e2, late, TN)
    mid[...] = (cot[...].astype(F32) + acc + jnp.concatenate([lo, hi], axis=1)).astype(BF)
    give = pltpu.make_async_remote_copy(
        src_ref=mid, dst_ref=midp, send_sem=ms, recv_sem=mr,
        device_id={"tp": 1 - tp}, device_id_type=MESH,
    )
    give.start()
    m1 = pltpu.make_async_copy(mid, mid_out.at[:, mine], od.at[7])
    m1.start()
    give.wait_recv()
    m2 = pltpu.make_async_copy(midp, mid_out.at[:, other], od.at[8])
    m2.start()
    for k in ORDER:
        out_copy(k).wait_send()
        pass_copy(k).wait_send()
        back_copy(k).wait_send()
    pass_copy(0).wait_send()
    swap.wait_send()
    give.wait_send()
    for c in outs + outs2 + [m1, m2]:
        c.wait()


def row_codes():
    code = np.full((NSP, 24, 2), -1.0, np.float32)
    back = np.full((NSP, 8, 3), -1.0, np.float32)
    for e in range(NSP):
        for u in range(8):
            code[e, u, 0] = code[e, 8 + u, 1] = e * CAP + u
            back[e, u, 0] = e * CAP + u
        for u in range(4):
            code[e, 16 + u, 0] = code[e, 20 + u, 1] = e * CAP + 8 + u
            back[e, u, 1] = back[e, 4 + u, 2] = e * CAP + 8 + u
    return code.reshape(NSP * 24, 2), back.reshape(NSP * 8, 3)


def experts(cotangent, mixed_input, route_ids, route_gates, wg, wu, wd):
    code, back = row_codes()
    dma = pltpu.SemaphoreType.DMA
    v = lambda *s: pltpu.VMEM(s, BF)
    rows = NSP * CAP
    out = lambda *s: jax.ShapeDtypeStruct(s, BF)
    return pl.pallas_call(
        expert_kernel,
        out_shape=(
            out(rows, D), out(rows, D), out(rows, FL), out(rows, FL), out(rows, FL), out(TOK, D),
        ),
        in_specs=[VM, VM, VM, VM, ANY, ANY, ANY, ANY, ANY],
        out_specs=(ANY,) * 6,
        scratch_shapes=[
            v(TOK, HD), v(TOK, HD), v(D, FL), v(D, FL), v(FL, D),
            v(192, 8, HD), v(192, 8, HD), v(192, 8, HD),
            v(rows, HD), v(rows, HD), v(rows, HD), v(rows, HD),
            v(rows, FL), v(rows, FL), v(rows, FL),
            v(rows, HD), v(rows, HD), v(rows, HD),
            v(NSP, 8, 1536), v(NSP, 8, 1536), v(TOK, HD), v(TOK, HD),
            dma((5,)), dma((NSP,)), dma((NSP,)), dma((NSP,)), dma((NSP,)), dma, dma,
            dma((NSP,)), dma((NSP,)), dma, dma, dma((9,)),
        ],
        compiler_params=pltpu.CompilerParams(
            collective_id=1, has_side_effects=True, vmem_limit_bytes=60 * 1024 * 1024
        ),
        name="experts",
    )(
        route_ids.T, route_gates.T, jnp.asarray(code), jnp.asarray(back),
        cotangent, mixed_input, wg, wu, wd,
    )


def halves(x):
    hi = x.astype(BF)
    return hi, (x - hi.astype(F32)).astype(BF)


def exact_left(ones, x, dims=NN):
    hi, lo = halves(x)
    rest = (x - hi.astype(F32) - lo.astype(F32)).astype(BF)
    return mm(ones, hi, dims) + mm(ones, lo, dims) + mm(ones, rest, dims)


def left2(x, b, dims):
    hi, lo = halves(x)
    return mm(hi, b, dims) + mm(lo, b, dims)


def right2(a, x, dims):
    hi, lo = halves(x)
    return mm(a, hi, dims) + mm(a, lo, dims)


def both3(a, b, dims):
    ah, al = halves(a)
    bh, bl = halves(b)
    return mm(ah, bh, dims) + mm(al, bh, dims) + mm(ah, bl, dims)


def iota(shape, dim):
    return lax.broadcasted_iota(jnp.int32, shape, dim)


def squeezed(top_of, low):
    return jnp.concatenate(
        [jnp.where(low, top_of(p)[0:32], top_of(p)[32:64]) for p in range(4)], axis=0
    )


def spread(comp, low):
    rows = []
    for p in range(4):
        c = comp[32 * p : 32 * p + 32]
        blk = jnp.concatenate([jnp.where(low, c, 0.0), jnp.where(low, 0.0, c)], axis=0)
        z = jnp.zeros((64, 128), F32)
        rows.append(jnp.concatenate([blk if j == p else z for j in range(4)], axis=1))
    return jnp.concatenate(rows, axis=0)


def mixer_kernel(
    mid_ref, proj_ref, mo_ref, q_ref, k_ref, v_ref, lf_ref, lb_ref,
    pg_out, q_out, k_out, v_out, f_out, b_out,
    g_s, pp, pin, st, sr, res, fin, qh, ql, kh, kl, dq_s, dk_s,
    ss, rs, s2, r2, s3, r3,
):
    sp, tp = lax.axis_index("sp"), lax.axis_index("tp")
    barrier = pltpu.get_barrier_semaphore()
    announce(sp, tp, barrier)
    scale = 32.0 ** -0.5
    rows_i, cols_i = iota((TOK, TOK), 0), iota((TOK, TOK), 1)
    lower = (cols_i <= rows_i).astype(F32).astype(BF)
    upper = (cols_i >= rows_i).astype(F32).astype(BF)
    lf, lb = lf_ref[...], lb_ref[...]
    pf, pb = exact_left(lower, lf), exact_left(upper, lb)
    tf, tb = pf[TOK - 1 : TOK], pb[0:1]
    cf, cb = pf[95:96], pb[96:97]
    qs = q_ref[...].astype(F32) * scale
    kv = k_ref[...].astype(F32)
    vals = v_ref[...]
    mix = mm(mid_ref[...], proj_ref[...]).astype(BF)
    g_s[...] = mix
    low = iota((32, 128), 1) < 64
    ones = jnp.ones((TOK, 128), BF)

    def wide(x, y):
        w = left2(x, y, TN)
        return squeezed(lambda p: w[64 * p : 64 * p + 64, 128 * p : 128 * p + 128], low)

    def decays(x):
        hi, lo = halves(x)
        rest = (x - hi.astype(F32) - lo.astype(F32)).astype(BF)
        w = jnp.exp(mm(hi, ones, TN) + mm(lo, ones, TN) + mm(rest, ones, TN))
        return squeezed(lambda p: w[64 * p : 64 * p + 64], low)

    kef, keb = kv * jnp.exp(tf - pf), kv * jnp.exp(tb - pb)
    df, db = decays(lf), decays(lb)
    maps = (
        wide(kef, vals), wide(keb, vals), wide(qs * jnp.exp(pf), mix), wide(qs * jnp.exp(pb), mix),
        df, db, df, db,
    )
    for j, m in enumerate(maps):
        for i in range(2):
            st[pl.ds(2 * j + i, NSP, stride=16), :] = m[64 * i : 64 * i + 64]
    pl.semaphore_wait(barrier, NSP)

    def state_copy(k):
        d = shifted(sp, comps(k))
        return pltpu.make_async_remote_copy(
            src_ref=st.at[pl.ds(pl.multiple_of(16 * d, 16), 16)],
            dst_ref=sr.at[pl.ds(pl.multiple_of(16 * sp, 16), 16)],
            send_sem=ss.at[k], recv_sem=rs.at[k], device_id={"sp": d}, device_id_type=MESH,
        )

    def result_copy(k):
        d = shifted(sp, comps(k))
        return pltpu.make_async_remote_copy(
            src_ref=res.at[pl.ds(pl.multiple_of(8 * d, 8), 8)],
            dst_ref=fin.at[pl.ds(pl.multiple_of(8 * sp, 8), 8)],
            send_sem=s2.at[k], recv_sem=r2.at[k], device_id={"sp": d}, device_id_type=MESH,
        )

    def proj_copy(k):
        d = shifted(sp, comps(k))
        return pltpu.make_async_remote_copy(
            src_ref=pp.at[d], dst_ref=pin.at[sp],
            send_sem=s3.at[k], recv_sem=r3.at[k], device_id={"sp": d}, device_id_type=MESH,
        )

    for k in ORDER:
        state_copy(k).start()
    own16 = pl.ds(pl.multiple_of(16 * sp, 16), 16)
    sr[own16, :] = st[own16, :]

    def part(i, c):
        cols = pl.ds(pl.multiple_of(i * 512, 512), 512)
        pp[pl.ds(16 * i, 16)] = mm(mid_ref[:, cols], mo_ref[...], TN).reshape(16, 32, FL).astype(BF)
        return c

    lax.fori_loop(0, 4, part, 0)
    for n, (p, c) in enumerate(((pf, cf), (pb, cb))):
        qh[n], ql[n] = halves(qs * jnp.exp(p - c))
        kh[n], kl[n] = halves(kv * jnp.exp(c - p))
    dq_s[...] = jnp.zeros_like(dq_s)
    dk_s[...] = jnp.zeros_like(dk_s)
    v_out[...] = jnp.zeros_like(v_out)
    lane = iota((TOK, 128), 1)

    def head(h, carry):
        pair = pl.ds(pl.multiple_of((h // 2) * 128, 128), 128)
        tile = pl.ds(pl.multiple_of((h // 4) * 128, 128), 128)
        half = (lane // 64) == h % 2
        quarter = (lane // 32) == h % 4
        gp, vp = g_s[:, pair], v_ref[:, pair]
        gh = jnp.where(half, gp, jnp.zeros_like(gp))
        da = mm(gh, vp, NT)
        dat = mm(vp, gh, NT)
        at = jnp.zeros((TOK, TOK), F32)
        for n in range(2):
            keep = cols_i <= rows_i if n == 0 else cols_i >= rows_i
            keep_t = cols_i >= rows_i if n == 0 else cols_i <= rows_i
            pick = lambda r: jnp.where(quarter, r[n, :, tile], jnp.zeros((TOK, 128), BF))
            a, b, c, d = pick(qh), pick(ql), pick(kh), pick(kl)
            s = mm(c, a, NT) + mm(c, b, NT) + mm(d, a, NT)
            at = at + jnp.where(keep_t, s, 0.0)
            hi, lo = halves(jnp.where(keep, da, 0.0))
            dq_s[n, :, tile] += mm(hi, c) + mm(hi, d) + mm(lo, c)
            hi, lo = halves(jnp.where(keep_t, dat, 0.0))
            dk_s[n, :, tile] += mm(hi, a) + mm(hi, b) + mm(lo, a)
        v_out[:, pair] += left2(at, gh, NN)
        return carry

    lax.fori_loop(0, 4, head, 0)
    for k in ORDER:
        state_copy(k).wait_recv()

    def up(s, u):
        at = pl.multiple_of(16 * s, 16)
        res[pl.ds(pl.multiple_of(8 * s, 8), 8), :] = u
        return sr[pl.ds(at + 8, 8), :] * u + sr[pl.ds(at, 8), :]

    r8 = iota((8, 128), 0)
    rising = (r8 < 2) | (r8 >= 6)

    def down(i, w):
        s = NSP - 1 - i
        at, to = pl.multiple_of(16 * s, 16), pl.ds(pl.multiple_of(8 * s, 8), 8)
        res[to, :] = jnp.where(rising, res[to, :], w)
        return sr[pl.ds(at + 8, 8), :] * w + sr[pl.ds(at, 8), :]

    zero = jnp.zeros((8, 128), F32)
    lax.fori_loop(0, NSP, up, zero)
    lax.fori_loop(0, NSP, down, zero)
    for k in ORDER:
        result_copy(k).start()
    own8 = pl.ds(pl.multiple_of(8 * sp, 8), 8)
    fin[own8, :] = res[own8, :]
    for k in ORDER:
        proj_copy(k).start()
    pin[sp] = pp[sp]
    lax.fori_loop(4, 8, head, 0)
    for k in ORDER:
        result_copy(k).wait_recv()

    def found(j):
        return spread(
            jnp.concatenate([fin[pl.ds(2 * j + i, NSP, stride=8), :] for i in range(2)], axis=0), low
        )

    sf, sb, gf, gb = found(0), found(1), found(2), found(3)
    ones8 = jnp.ones((8, FL), BF)
    dqs, dks = 0.0, 0.0
    for n, (p, c, t, ke, s, g, sums, out) in enumerate(
        ((pf, cf, tf, kef, sf, gf, upper, f_out), (pb, cb, tb, keb, sb, gb, lower, b_out))
    ):
        dq = jnp.exp(p - c) * dq_s[n] + jnp.exp(p) * right2(mix, s, NT)
        ik = jnp.exp(t - p) * right2(vals, g, NT)
        dk = jnp.exp(c - p) * dk_s[n] + ik
        both = exact_left(ones8, s * g, NT)[0:1]
        total = jnp.exp(t) * both + jnp.sum(kv * ik, axis=0, keepdims=True)
        out[...] = exact_left(sums, qs * dq - kv * dk) + total
        v_out[...] += both3(ke, g, NN)
        dqs, dks = dqs + dq, dks + dk
    q_out[...] = dqs * scale
    k_out[...] = dks
    for k in ORDER:
        proj_copy(k).wait_recv()

    def add(i, acc):
        return acc + pin[i].astype(F32)

    pg_out[...] = lax.fori_loop(0, NSP, add, jnp.zeros((32, FL), F32))
    for k in ORDER:
        state_copy(k).wait_send()
        result_copy(k).wait_send()
        proj_copy(k).wait_send()


def mixer(mid, proj, mo, q, k, v, lf, lb):
    dma = pltpu.SemaphoreType.DMA
    f = lambda *s: jax.ShapeDtypeStruct(s, F32)
    vb = lambda *s: pltpu.VMEM(s, BF)
    vf = lambda *s: pltpu.VMEM(s, F32)
    return pl.pallas_call(
        mixer_kernel,
        out_shape=(f(32, FL), f(TOK, 256), f(TOK, 256), f(TOK, FL), f(TOK, 256), f(TOK, 256)),
        in_specs=[VM] * 8,
        out_specs=(VM,) * 6,
        scratch_shapes=[
            vb(TOK, FL), vb(NSP, 32, FL), vb(NSP, 32, FL), vf(1024, 128), vf(1024, 128),
            vf(512, 128), vf(512, 128), vb(2, TOK, 256), vb(2, TOK, 256), vb(2, TOK, 256),
            vb(2, TOK, 256), vf(2, TOK, 256), vf(2, TOK, 256),
        ]
        + [dma((NSP,))] * 6,
        compiler_params=pltpu.CompilerParams(
            collective_id=2, has_side_effects=True, vmem_limit_bytes=56 * 1024 * 1024
        ),
        name="mixer",
    )(mid, proj, mo, q, k, v, lf, lb)


def local(
    cotangent, mixed_input, route_ids, route_gates, expert_gate, expert_up, expert_down,
    projection, mixer_output, query_rows, key_rows, value_rows, log_forward, log_backward,
):
    c, t, h, gg, ug, mid = experts(
        cotangent, mixed_input, route_ids, route_gates, expert_gate[0], expert_up[0], expert_down[0]
    )
    rest = mixer(
        mid, projection, mixer_output, query_rows, key_rows, value_rows, log_forward, log_backward
    )
    return (mm(t, gg, TN)[None], mm(t, ug, TN)[None], mm(h, c, TN)[None], *rest)


def solution(mesh):
    sp, tok = P("sp", None), P("sp", "tp")
    ein, eout = P("sp", None, "tp"), P("sp", "tp", None)
    return jax.shard_map(
        local,
        mesh=mesh,
        in_specs=(sp, sp, sp, sp, ein, ein, eout, P(None, "tp")) + (tok,) * 6,
        out_specs=(ein, ein, eout) + (tok,) * 6,
        check_vma=False,
    )
```
